32 devices in a mesh: sp: 8 (over z, x), tp: 4 (over y, core).
Axes of the slice: x: 2, y: 2, z: 4, core: 2. Of those that a mesh axis runs over, the one named last changes fastest.
Arguments:
- residual: bfloat16 [1024, 2048], P(('sp', 'tp')), may hold values from -20 to 20
- query_small: bfloat16 [1024, 384], P('sp', 'tp'), may hold values from -12 to 12
- query_large: bfloat16 [1024, 640], P('sp', 'tp'), may hold values from -12 to 12
- latent: bfloat16 [1024, 512], P('sp'), may hold values from -30 to 30
- rotary_key: bfloat16 [1024, 32], P('sp'), may hold values from -16 to 16
- latent_gain: float32 [512], replicated, may hold values from 0.1 to 1.9
- small_keys: bfloat16 [512, 256], P(None, 'tp'), may hold values from -0.25 to 0.25
- small_values: bfloat16 [512, 256], P(None, 'tp'), may hold values from -0.25 to 0.25
- large_keys: bfloat16 [512, 512], P(None, 'tp'), may hold values from -0.25 to 0.25
- large_values: bfloat16 [512, 512], P(None, 'tp'), may hold values from -0.25 to 0.25
- small_output: bfloat16 [256, 2048], P('tp'), may hold values from -0.21875 to 0.21875
- large_output: bfloat16 [512, 2048], P('tp'), may hold values from -0.21875 to 0.21875
- ffn_gain: float32 [2048], replicated, may hold values from 0.1 to 1.9
- gate_weights: bfloat16 [8, 2048, 2048], P('sp', None, 'tp'), may hold values from -2 to 2
- up_weights: bfloat16 [8, 2048, 2048], P('sp', None, 'tp'), may hold values from -2 to 2
- down_weights: bfloat16 [8, 2048, 2048], P('sp', 'tp'), may hold values from -0.046875 to 0.046875
- routing: int32 [1024, 2], P(('sp', 'tp')), may hold values from 0 to 7, all different within a row; in each aligned block of 32 rows (0 to 31, 32 to 63, ...) at most 16 rows name the same one
- route_weight: float32 [1024, 2], P(('sp', 'tp')), may hold values from 0.2 to 1
Outputs:
- output: bfloat16 [1024, 2048], P(('sp', 'tp'))
The draws below stay inside these ranges and needn't reach their ends.
Inputs may be any that keep to these rules, and one draw needn't show every extreme that they name: `routing`: each row names 2 different experts. Within the rows of one device (aligned blocks of 32 rows) no expert is named by more than 16 rows, and in every draw some block has an expert named by exactly 16 rows.
All inputs are finite; a program needn't handle non-finite values.
Results may differ from the reference program's by a relative error of at most 0.018.
Values may be sent and summed in bfloat16 or wider, within the bound.
A program may use at most 128 MiB of HBM per device.

```python
import math
import jax
import jax.numpy as jnp
import numpy as np
from jax import lax

D = 2048
LATENT = 512
HEADS_S = 4
HEADS_L = 4
NOPE_S = 64
V_S = 64
NOPE_L = 128
V_L = 128
ROPE = 32
FF = 2048
TOPK = 2
TOK_DEV = 32
SEQ_LEN = 1024
EXPERTS = 8
CAP = 16
N_SP = 8
N_TP = 4


def scaled_rows(key, row_count, col_count, row_low, row_high, col_low, col_high):
    sub_keys = jax.random.split(jax.random.fold_in(key, 11), 3)
    base = jnp.clip(jax.random.normal(sub_keys[0], (row_count, col_count), jnp.float32), -5.0, 5.0)
    row_scale = jnp.exp(jax.random.uniform(sub_keys[1], (row_count, 1), jnp.float32, math.log(row_low), math.log(row_high)))
    col_scale = jnp.exp(jax.random.uniform(sub_keys[2], (1, col_count), jnp.float32, math.log(col_low), math.log(col_high)))
    return base * row_scale * col_scale


def draw_queries(key, head_count, nope, salt):
    width = nope + ROPE
    own_key = jax.random.fold_in(key, salt)
    whole = jnp.clip(2.5 * jax.random.normal(own_key, (SEQ_LEN, head_count, width), jnp.float32), -12.0, 12.0)
    return whole.reshape(SEQ_LEN, head_count * width)


def draw_query_small(key, part):
    return draw_queries(key, HEADS_S, NOPE_S, 21).astype(jnp.bfloat16)


def draw_query_large(key, part):
    return draw_queries(key, HEADS_L, NOPE_L, 22).astype(jnp.bfloat16)


def draw_rotary_key(key, part):
    own_key = jax.random.fold_in(key, 31)
    base = jnp.clip(jax.random.normal(own_key, (SEQ_LEN, ROPE), jnp.float32), -6.0, 6.0)
    return base.astype(jnp.bfloat16)


def draw_residual(key, part):
    return scaled_rows(jax.random.fold_in(key, 41), SEQ_LEN, D, 0.5, 2.0, 0.5, 2.0).astype(jnp.bfloat16)


def draw_latent(key, part):
    return scaled_rows(jax.random.fold_in(key, 42), SEQ_LEN, LATENT, 0.3, 3.0, 0.5, 2.0).astype(jnp.bfloat16)


def expert_matrix(key, salt):
    own_key = jax.random.fold_in(key, salt)
    return jnp.clip(jax.random.normal(own_key, (EXPERTS, D, FF), jnp.float32), -6.0, 6.0) * (2.5 / math.sqrt(D))


def draw_gate_weights(key, part):
    return expert_matrix(key, 51).astype(jnp.bfloat16)


def draw_up_weights(key, part):
    return expert_matrix(key, 52).astype(jnp.bfloat16)


def block_levels(stream_key, dims, cuts, low, high):
    level = 1.0
    for position, parts in cuts:
        draws = jax.random.uniform(jax.random.fold_in(jax.random.fold_in(stream_key, 6), position), (parts,), jnp.float32, low / len(cuts), high / len(cuts))
        level = level * jnp.repeat(jnp.exp(draws), dims[position] // parts).reshape((-1,) + (1,) * (len(dims) - 1 - position))
    return level


def shared_out(key, own, number, rows, count, top, reach, skew):
    order = jax.random.permutation(key, count)
    crowded, ordinary = load_shares(count, rows * top, reach, skew, True), load_shares(count, rows * top, reach, skew, False)
    places = jnp.arange(count)

    def named(lengths, offset_by):
        used = int((lengths > 0).sum())
        fixed = max(1, used // 4)
        moved = fixed + (places - fixed + offset_by * (used - fixed)) % max(1, count - fixed)
        return jnp.zeros((count,), jnp.int32).at[order[jnp.where(places < fixed, places, moved)]].set(jnp.asarray(lengths, jnp.int32))

    lengths = jnp.where(number % 4 == 0, named(crowded, number // 4), named(ordinary, number - number // 4 - 1))
    mixed = jax.random.permutation(jax.random.fold_in(own, 3), count)
    source_of, receiver = mixed[0:count // 2 * 2:2], mixed[1:count // 2 * 2:2]
    slack = jnp.minimum(lengths[source_of] - 1, reach - lengths[receiver]) // 2
    slack = jnp.where((source_of == order[0]) | (receiver == order[0]) | (lengths[receiver] == 0), 0, jnp.maximum(slack, 0))
    moved = jax.random.randint(jax.random.fold_in(own, 4), (count // 2,), 0, 1 << 20) % (slack + 1)
    lengths = lengths.at[source_of].add(-moved).at[receiver].add(moved)
    labels = jnp.searchsorted(jnp.cumsum(lengths), jnp.arange(rows * top), side="right").astype(jnp.int32)
    table = labels.reshape(top, rows).T
    table = table[jax.random.permutation(jax.random.fold_in(own, 1), rows)]
    offset_by = jax.random.randint(jax.random.fold_in(own, 2), (rows, 1), 0, top)
    return jnp.take_along_axis(table, (jnp.arange(top)[None, :] + offset_by) % top, axis=1)


def load_shares(amount, total, reach, lean, full):
    portions = [(1 << 20) // math.isqrt(rank ** lean) + 1 for rank in range(1, amount + 1)]
    largest = reach if full else min(reach, max(-(-total // amount), total * portions[0] // sum(portions)))
    least = 1 if total - largest >= amount - 1 else 0
    holding, surplus = [largest] + [least] * (amount - 1), total - largest - least * (amount - 1)
    while surplus > 0:
        free = [i for i in range(1, amount) if holding[i] < largest] or [i for i in range(1, amount) if holding[i] < reach]
        whole, budget = sum([portions[i] for i in free]), surplus
        for i in free:
            extra = min(reach - holding[i], max(1, budget * portions[i] // whole), surplus)
            holding[i] = holding[i] + extra
            surplus = surplus - extra
    return np.array(holding)


def scatter_about(key, extent, deviation, limit, pieces=(), kind=jnp.bfloat16):
    entries = jax.random.normal(key, extent, jnp.float32) * deviation
    if len(pieces) > 0:
        entries = block_levels(key, extent, pieces, -0.22, 0.18) * entries
    return jnp.clip(entries, min=-limit, max=limit).astype(kind)


def setup_inputs(seed: int = 0) -> dict:
    splits = jax.random.split(jax.random.key(seed), 19)
    residual = draw_residual(jax.random.fold_in(splits[18], 71), 0)
    query_small = draw_query_small(jax.random.fold_in(splits[18], 71), 0)
    query_large = draw_query_large(jax.random.fold_in(splits[18], 71), 0)
    latent = draw_latent(jax.random.fold_in(splits[18], 71), 0)
    rotary_key = draw_rotary_key(jax.random.fold_in(splits[18], 71), 0)
    latent_gain = jnp.clip(1.0 + 0.18 * jax.random.normal(splits[5], (LATENT,), jnp.float32), 0.1, 1.9)
    small_keys = scatter_about(splits[6], (LATENT, HEADS_S * NOPE_S), LATENT ** -0.5, 0.25, ((1, 4),))
    small_values = scatter_about(splits[7], (LATENT, HEADS_S * V_S), LATENT ** -0.5, 0.25, ((1, 4),))
    large_keys = scatter_about(splits[8], (LATENT, HEADS_L * NOPE_L), LATENT ** -0.5, 0.25, ((1, 4),))
    large_values = scatter_about(splits[9], (LATENT, HEADS_L * V_L), LATENT ** -0.5, 0.25, ((1, 4),))
    small_output = scatter_about(splits[10], (HEADS_S * V_S, D), (HEADS_S * V_S + HEADS_L * V_L) ** -0.5, 0.21875, ((0, 4),))
    large_output = scatter_about(splits[11], (HEADS_L * V_L, D), (HEADS_S * V_S + HEADS_L * V_L) ** -0.5, 0.21875, ((0, 4),))
    ffn_gain = jnp.clip(1.0 + 0.18 * jax.random.normal(splits[12], (D,), jnp.float32), 0.1, 1.9)
    gate_weights = draw_gate_weights(jax.random.fold_in(splits[18], 71), 0)
    up_weights = draw_up_weights(jax.random.fold_in(splits[18], 71), 0)
    down_weights = scatter_about(splits[15], (EXPERTS, FF, D), (9 * FF) ** -0.5, 0.046875, ((0, 8), (1, 4)))
    routing_keys = jax.random.split(jax.random.fold_in(splits[16], 1), SEQ_LEN // TOK_DEV)
    routing_turns = jax.random.permutation(jax.random.fold_in(splits[16], 3), SEQ_LEN // TOK_DEV)
    routing = jax.vmap(lambda own, number: shared_out(jax.random.fold_in(splits[16], 2), own, number, TOK_DEV, EXPERTS, TOPK, CAP, 2))(routing_keys, routing_turns).reshape((SEQ_LEN, TOPK))
    route_weight = jnp.clip(jnp.exp(math.log(1.0) - 1.609438 * jax.random.uniform(splits[17], (SEQ_LEN, TOPK), jnp.float32) ** block_levels(splits[17], (SEQ_LEN, TOPK), ((0, 32),), -0.2, 0.2)), 0.2, 1.0)
    return {"residual": residual, "query_small": query_small, "query_large": query_large, "latent": latent, "rotary_key": rotary_key, "latent_gain": latent_gain, "small_keys": small_keys, "small_values": small_values, "large_keys": large_keys, "large_values": large_values, "small_output": small_output, "large_output": large_output, "ffn_gain": ffn_gain, "gate_weights": gate_weights, "up_weights": up_weights, "down_weights": down_weights, "routing": routing, "route_weight": route_weight}


eps = 1e-06
clamp_limit = 7.0
glu_alpha = 1.702
rope_base = 10000.0
masked_score = -1e+30

def rope_tables(row_count, first_pos):
    half_size = ROPE // 2
    frequencies = jnp.power(rope_base, -jnp.arange(half_size, dtype=jnp.float32) * (2.0 / ROPE))
    places = (first_pos + jnp.arange(row_count, dtype=jnp.int32)).astype(jnp.float32)
    angles = places[:, None] * frequencies[None, :]
    return (jnp.cos(angles), jnp.sin(angles))

def rotate(values_in, cos_vals, sin_vals):
    front_half, back_half = jnp.split(values_in, 2, axis=-1)
    return jnp.concatenate([front_half * cos_vals - back_half * sin_vals, back_half * cos_vals + front_half * sin_vals], axis=-1)

def rms_scaled(values_in, gain):
    widened = values_in.astype(jnp.float32)
    return widened * lax.rsqrt(lax.optimization_barrier(jnp.mean(widened * widened, axis=-1, keepdims=True)) + eps) * gain

def turn_queries(query, nope, cos_vals, sin_vals):
    width = nope + ROPE
    shaped = query.reshape(query.shape[0], query.shape[1] // width, width)
    turned = rotate(shaped[:, :, nope:].astype(jnp.float32), cos_vals[:, None, :], sin_vals[:, None, :])
    return jnp.concatenate([shaped[:, :, :nope], turned.astype(jnp.bfloat16)], axis=2)

def clamped(gate_pre, up_pre):
    limited = jnp.minimum(gate_pre, clamp_limit)
    linear = jnp.clip(up_pre, -clamp_limit, clamp_limit)
    return limited * jax.nn.sigmoid(glu_alpha * limited) * (linear + 1.0)

def attend_group(query, keys_in, values_in, rotary, nope):
    seq_rows = query.shape[0]
    head_count = query.shape[1]
    key_heads = keys_in.reshape(seq_rows, head_count, nope).astype(jnp.float32)
    value_heads = values_in.reshape(seq_rows, head_count, -1).astype(jnp.float32)
    rotary_wide = rotary.astype(jnp.float32)
    block_rows = math.gcd(seq_rows, 512)
    blocks = query.reshape(seq_rows // block_rows, block_rows, head_count, nope + ROPE)
    key_pos = jnp.arange(seq_rows, dtype=jnp.int32)

    def one_block(inputs):
        query_block, block_index = inputs
        query_wide = query_block.astype(jnp.float32)
        scores = jnp.einsum('qhd,khd->hqk', query_wide[:, :, :nope], key_heads)
        scores = scores + jnp.einsum('qhd,kd->hqk', query_wide[:, :, nope:], rotary_wide)
        query_pos = block_index * block_rows + jnp.arange(block_rows, dtype=jnp.int32)
        allowed = key_pos[None, :] <= query_pos[:, None]
        scores = jnp.where(allowed[None], scores * (nope + ROPE) ** (-0.5), masked_score)
        top_score = lax.optimization_barrier(jnp.max(scores, axis=2, keepdims=True))
        weights = jnp.exp(scores - top_score)
        weight_sum = lax.optimization_barrier(jnp.sum(weights, axis=2))
        rounded = lax.optimization_barrier(weights.astype(jnp.bfloat16)).astype(jnp.float32)
        mixed = jnp.einsum('hqk,khd->qhd', rounded, value_heads)
        return (mixed / weight_sum.T[:, :, None]).reshape(block_rows, -1).astype(jnp.bfloat16)
    outputs = lax.map(one_block, (blocks, jnp.arange(seq_rows // block_rows, dtype=jnp.int32)))
    return outputs.reshape(seq_rows, -1)

def expert_outputs(normed, routing, gate_weights, up_weights, down_weights):
    device_count = N_SP * N_TP
    assigned = routing.reshape(device_count, TOK_DEV * TOPK)
    onehot = (assigned[:, :, None] == jnp.arange(EXPERTS, dtype=jnp.int32)[None, None, :]).astype(jnp.int32)
    slot_index = lax.optimization_barrier(jnp.sum((jnp.cumsum(onehot, axis=1) - onehot) * onehot, axis=2))
    width_all = device_count * CAP
    places = assigned * width_all + jnp.arange(device_count, dtype=jnp.int32)[:, None] * CAP + slot_index
    places = places.reshape(-1).astype(jnp.int32)
    slot_table = jnp.full((EXPERTS * width_all,), -1, jnp.int32)
    slot_table = slot_table.at[places].set(jnp.arange(places.shape[0], dtype=jnp.int32))
    slot_table = slot_table.reshape(EXPERTS, width_all)
    run_width = FF // N_TP

    def one_expert(inputs):
        index_row, gate_one, up_one, down_one = inputs
        rows_in = normed[jnp.maximum(index_row, 0) // TOPK]
        gate_pre = jnp.dot(rows_in, gate_one, preferred_element_type=jnp.float32)
        up_pre = jnp.dot(rows_in, up_one, preferred_element_type=jnp.float32)
        hidden = clamped(gate_pre, up_pre).astype(jnp.bfloat16)
        summed = jnp.zeros((rows_in.shape[0], D), jnp.float32)
        for group_index in range(N_TP):
            lower = group_index * run_width
            partial_sum = jnp.dot(hidden[:, lower:lower + run_width], down_one[lower:lower + run_width], preferred_element_type=jnp.float32)
            summed = summed + lax.optimization_barrier(partial_sum.astype(jnp.bfloat16)).astype(jnp.float32)
        return summed.astype(jnp.bfloat16)
    outputs = lax.map(one_expert, (slot_table, gate_weights, up_weights, down_weights))
    return outputs.reshape(-1, D)[places]

def reference(residual, query_small, query_large, latent, rotary_key, latent_gain, small_keys, small_values, large_keys, large_values, small_output, large_output, ffn_gain, gate_weights, up_weights, down_weights, routing, route_weight):
    seq_rows = latent.shape[0]
    cos_vals, sin_vals = rope_tables(seq_rows, 0)
    small_query = turn_queries(query_small, NOPE_S, cos_vals, sin_vals)
    large_query = turn_queries(query_large, NOPE_L, cos_vals, sin_vals)
    normed_latent = rms_scaled(latent, latent_gain).astype(jnp.bfloat16)
    projected = [jnp.dot(normed_latent, weight, preferred_element_type=jnp.float32).astype(jnp.bfloat16) for weight in (small_keys, small_values, large_keys, large_values)]
    rotary = rotate(rotary_key.astype(jnp.float32), cos_vals, sin_vals).astype(jnp.bfloat16)
    small_heads = attend_group(small_query, projected[0], projected[1], rotary, NOPE_S)
    large_heads = attend_group(large_query, projected[2], projected[3], rotary, NOPE_L)
    small_span = HEADS_S // N_TP * V_S
    large_span = HEADS_L // N_TP * V_L
    summed = jnp.zeros((seq_rows, D), jnp.float32)
    for group_index in range(N_TP):
        small_low = group_index * small_span
        large_low = group_index * large_span
        partial_sum = jnp.dot(small_heads[:, small_low:small_low + small_span], small_output[small_low:small_low + small_span], preferred_element_type=jnp.float32)
        partial_sum = partial_sum + jnp.dot(large_heads[:, large_low:large_low + large_span], large_output[large_low:large_low + large_span], preferred_element_type=jnp.float32)
        summed = summed + lax.optimization_barrier(partial_sum.astype(jnp.bfloat16)).astype(jnp.float32)
    attention = lax.optimization_barrier(summed.astype(jnp.bfloat16)).astype(jnp.float32)
    middle = lax.optimization_barrier((residual.astype(jnp.float32) + attention).astype(jnp.bfloat16))
    normed = rms_scaled(middle, ffn_gain).astype(jnp.bfloat16)
    picked = expert_outputs(normed, routing, gate_weights, up_weights, down_weights)
    mixed = lax.optimization_barrier(jnp.sum(route_weight[:, :, None] * picked.astype(jnp.float32).reshape(seq_rows, TOPK, D), axis=1))
    return (middle.astype(jnp.float32) + mixed).astype(jnp.bfloat16)
```

```python
import functools

import jax
import jax.numpy as jnp
from jax import lax
from jax.experimental import pallas as pl
from jax.experimental.pallas import tpu as pltpu
from jax.sharding import PartitionSpec as P

NOPE_S = 64
NOPE_L = 128
ROPE = 32
TOPK = 2


eps = 1e-06
clamp_limit = 7.0
glu_alpha = 1.702
rope_base = 10000.0
masked_score = -1e30


def rope_tables(row_count, first_pos):
    half_size = ROPE // 2
    frequencies = jnp.power(rope_base, -jnp.arange(half_size, dtype=jnp.float32) * (2.0 / ROPE))
    places = (first_pos + jnp.arange(row_count, dtype=jnp.int32)).astype(jnp.float32)
    angles = places[:, None] * frequencies[None, :]
    return (jnp.cos(angles), jnp.sin(angles))


def rotate(values_in, cos_vals, sin_vals):
    front_half, back_half = jnp.split(values_in, 2, axis=-1)
    return jnp.concatenate(
        [
            front_half * cos_vals - back_half * sin_vals,
            back_half * cos_vals + front_half * sin_vals,
        ],
        axis=-1,
    )


def rms_scaled(values_in, gain):
    widened = values_in.astype(jnp.float32)
    return widened * lax.rsqrt(jnp.mean(widened * widened, axis=-1, keepdims=True) + eps) * gain


def turn_queries(query, nope, cos_vals, sin_vals):
    width = nope + ROPE
    shaped = query.reshape(query.shape[0], query.shape[1] // width, width)
    turned = rotate(
        shaped[:, :, nope:].astype(jnp.float32), cos_vals[:, None, :], sin_vals[:, None, :]
    )
    return jnp.concatenate([shaped[:, :, :nope], turned.astype(jnp.bfloat16)], axis=2)


def clamped(gate_pre, up_pre):
    limited = jnp.minimum(gate_pre, clamp_limit)
    linear = jnp.clip(up_pre, -clamp_limit, clamp_limit)
    return limited * jax.nn.sigmoid(glu_alpha * limited) * (linear + 1.0)


def make_keys(latent_rows, raw_rotary, first_pos, latent_gain, projections):
    normed_latent = rms_scaled(latent_rows, latent_gain).astype(jnp.bfloat16)
    projected = tuple(
        (
            jnp.dot(normed_latent, weight, preferred_element_type=jnp.float32).astype(jnp.bfloat16)
            for weight in projections
        )
    )
    cos_vals, sin_vals = rope_tables(latent_rows.shape[0], first_pos)
    turned = rotate(raw_rotary.astype(jnp.float32), cos_vals, sin_vals).astype(jnp.bfloat16)
    return projected + (turned,)


def empty_state(query, values_in):
    head_count = query.shape[1]
    row_count = query.shape[0]
    value_size = values_in.shape[1] // head_count
    return (
        jnp.full((head_count, row_count), masked_score, jnp.float32),
        jnp.zeros((head_count, row_count), jnp.float32),
        jnp.zeros((row_count, head_count, value_size), jnp.float32),
    )


def update(state_now, query, keys_in, values_in, rotary, nope, allowed):
    running_max, weight_sum, weighted = state_now
    head_count = query.shape[1]
    span_rows = rotary.shape[0]
    key_heads = keys_in.reshape(span_rows, head_count, nope)
    value_heads = values_in.reshape(span_rows, head_count, -1)
    scores = jnp.einsum(
        "rhd,khd->hrk", query[:, :, :nope], key_heads, preferred_element_type=jnp.float32
    )
    scores = scores + jnp.einsum(
        "rhd,kd->hrk", query[:, :, nope:], rotary, preferred_element_type=jnp.float32
    )
    scores = jnp.where(allowed[None], scores * (nope + ROPE) ** (-0.5), masked_score)
    new_max = jnp.maximum(running_max, jnp.max(scores, axis=2))
    weights = jnp.where(allowed[None], jnp.exp(scores - new_max[:, :, None]), 0.0)
    rescale = jnp.exp(running_max - new_max)
    weight_sum = jnp.sum(weights, axis=2)
    weighted = weighted * rescale.T[:, :, None] + jnp.einsum(
        "hrk,khd->rhd",
        weights.astype(jnp.bfloat16),
        value_heads,
        preferred_element_type=jnp.float32,
    )
    return (new_max, weight_sum, weighted)


def finish(state_end, row_count):
    running_max, weight_sum, weighted = state_end
    return (weighted / weight_sum.T[:, :, None]).reshape(row_count, -1).astype(jnp.bfloat16)


def on_device(
    residual,
    query_small,
    query_large,
    latent,
    rotary_key,
    latent_gain,
    small_keys,
    small_values,
    large_keys,
    large_values,
    small_output,
    large_output,
    ffn_gain,
    gate_weights,
    up_weights,
    down_weights,
    routing,
    route_weight,
):
    row_count = latent.shape[0]
    first_pos = lax.axis_index("sp") * row_count
    cos_vals, sin_vals = rope_tables(row_count, first_pos)
    small_query = turn_queries(query_small, NOPE_S, cos_vals, sin_vals)
    large_query = turn_queries(query_large, NOPE_L, cos_vals, sin_vals)
    query_pos = first_pos + jnp.arange(row_count, dtype=jnp.int32)
    last_pos = first_pos + row_count - 1
    projections = (small_keys, small_values, large_keys, large_values)
    initial = (empty_state(small_query, small_values), empty_state(large_query, large_values))

    def from_latent(key_set, offset):
        return make_keys(key_set[0], key_set[1], offset, latent_gain, projections)

    key_set = (
        lax.all_gather(latent, "sp", axis=0, tiled=True),
        lax.all_gather(rotary_key, "sp", axis=0, tiled=True),
    )
    offset = jnp.int32(0)
    span_rows = key_set[0].shape[0]
    allowed = jnp.arange(span_rows, dtype=jnp.int32)[None, :] <= query_pos[:, None]

    def live(inner):
        ready = from_latent(key_set, offset)
        return (
            update(inner[0], small_query, ready[0], ready[1], ready[4], NOPE_S, allowed),
            update(inner[1], large_query, ready[2], ready[3], ready[4], NOPE_L, allowed),
        )

    def keep_state(inner):
        return inner

    state_end = lax.cond(offset <= last_pos, live, keep_state, initial)
    small_heads = finish(state_end[0], row_count)
    large_heads = finish(state_end[1], row_count)
    tok_count = row_count // lax.axis_size("tp")
    summed = lax.psum_scatter(
        (
            jnp.dot(small_heads, small_output, preferred_element_type=jnp.float32)
            + jnp.dot(large_heads, large_output, preferred_element_type=jnp.float32)
        ).astype(jnp.bfloat16),
        "tp",
        scatter_dimension=0,
        tiled=True,
    )
    attention = lax.optimization_barrier(summed).astype(jnp.float32)
    middle = lax.optimization_barrier(
        (residual.astype(jnp.float32) + attention).astype(jnp.bfloat16)
    )
    normed = rms_scaled(middle, ffn_gain).astype(jnp.bfloat16)
    local_experts = gate_weights.shape[0]
    expert_count = local_experts * lax.axis_size("sp")
    capacity = max(2, 2 * TOPK * tok_count // expert_count)
    assigned = routing.reshape(-1)
    onehot = (assigned[:, None] == jnp.arange(expert_count, dtype=jnp.int32)[None, :]).astype(
        jnp.int32
    )
    slot_index = jnp.sum((jnp.cumsum(onehot, axis=0) - onehot) * onehot, axis=1)
    places = assigned * capacity + slot_index
    pick_table = (
        places[:, None] == jnp.arange(expert_count * capacity, dtype=jnp.int32)[None, :]
    ).astype(jnp.bfloat16)
    send_table = jnp.sum(pick_table.reshape(tok_count, TOPK, -1), axis=1)
    outgoing = lax.dot_general(
        send_table, normed, (((0,), (0,)), ((), ())), preferred_element_type=jnp.float32
    )
    outgoing = outgoing.astype(jnp.bfloat16).reshape(expert_count, capacity, -1)
    shard_piece = lax.all_gather(
        lax.all_to_all(outgoing, "sp", split_axis=0, concat_axis=0, tiled=True),
        "tp",
        axis=0,
        tiled=True,
    )
    grouped = shard_piece.reshape(-1, local_experts, shard_piece.shape[1], shard_piece.shape[2])
    gate_pre = jnp.einsum(
        "secd,edf->secf", grouped, gate_weights, preferred_element_type=jnp.float32
    )
    up_pre = jnp.einsum("secd,edf->secf", grouped, up_weights, preferred_element_type=jnp.float32)
    hidden = clamped(gate_pre, up_pre).astype(jnp.bfloat16)
    result = jnp.einsum("secf,efd->secd", hidden, down_weights, preferred_element_type=jnp.float32)
    partials = result.reshape(shard_piece.shape[0], shard_piece.shape[1], -1)
    combined = lax.psum_scatter(
        partials.astype(jnp.bfloat16), "tp", scatter_dimension=0, tiled=True
    )
    returned = lax.all_to_all(combined, "sp", split_axis=0, concat_axis=0, tiled=True)
    picked = jnp.dot(
        pick_table,
        returned.reshape(expert_count * capacity, -1),
        preferred_element_type=jnp.float32,
    )
    mixed = jnp.sum(route_weight[:, :, None] * picked.reshape(tok_count, TOPK, -1), axis=1)
    return (middle.astype(jnp.float32) + mixed).astype(jnp.bfloat16)


MESH_ID = pl.DeviceIdType.MESH


def remote(src, dst, send_sem, recv_sem, sp, tp):
    return pltpu.make_async_remote_copy(
        src_ref=src,
        dst_ref=dst,
        send_sem=send_sem,
        recv_sem=recv_sem,
        device_id=(sp, tp),
        device_id_type=MESH_ID,
    )


def rows_at(index, count):
    return pl.ds(pl.multiple_of(index * count, count), count)


def greet(n_sp, tp_peers, me_s, me_t):
    barrier = pltpu.get_barrier_semaphore()
    for step in range(1, n_sp):
        pl.semaphore_signal(
            barrier, inc=1, device_id=((me_s + step) % n_sp, me_t), device_id_type=MESH_ID
        )
    for peer in tp_peers:
        pl.semaphore_signal(barrier, inc=1, device_id=(me_s, peer), device_id_type=MESH_ID)
    pl.semaphore_wait(barrier, n_sp - 1 + len(tp_peers))


def dot_t(lhs, rhs):
    return lax.dot_general(
        lhs, rhs, (((1,), (1,)), ((), ())), preferred_element_type=jnp.float32
    )


def attention_kernel(
    n_sp,
    n_tp,
    scale_s,
    scale_l,
    pack_ref,
    qs_ref,
    ql_ref,
    proj_ref,
    out_s_ref,
    out_l_ref,
    residual_ref,
    middle_ref,
    lat,
    max_s,
    sum_s,
    acc_s,
    max_l,
    sum_l,
    acc_l,
    part,
    got,
    a_send,
    a_recv,
    y_send,
    y_recv,
    c_send,
    c_recv,
    d_send,
    d_recv,
    p_send,
    p_recv,
):
    me_s = lax.axis_index("sp")
    me_t = lax.axis_index("tp")
    core_t = me_t + 1 - 2 * (me_t % 2)
    y_t = (me_t + 2) % n_tp
    far_t = (core_t + 2) % n_tp
    rows = pack_ref.shape[0]
    latent_size = proj_ref.shape[0]
    quarter = rows // n_tp
    greet(n_sp, (core_t, y_t, far_t), me_s, me_t)

    def gather_copy(step, source, target):
        return remote(
            pack_ref.at[rows_at(me_t, quarter), :],
            lat.at[source, rows_at(me_t, quarter), :],
            a_send.at[step - 1],
            a_recv.at[step - 1],
            target,
            me_t,
        )

    def y_copy(step, source, owner):
        where = lat.at[source, rows_at(owner, quarter), :]
        return remote(where, where, y_send.at[step - 1], y_recv.at[step - 1], me_s, y_t)

    def c_copy(step, source, owner):
        where = lat.at[source, rows_at(owner, quarter), :]
        return remote(where, where, c_send.at[step - 1], c_recv.at[step - 1], me_s, core_t)

    def d_copy(step, source, owner):
        where = lat.at[source, rows_at(owner, quarter), :]
        return remote(where, where, d_send.at[step - 1], d_recv.at[step - 1], me_s, core_t)

    def send_on(step, carry):
        gather_copy(step, me_s, me_s + step).start()
        return carry

    lax.fori_loop(1, n_sp - me_s, send_on, 0)

    def span(block, first):
        projected = jnp.dot(
            block[:, :latent_size], proj_ref[...], preferred_element_type=jnp.float32
        ).astype(jnp.bfloat16)
        tile = projected.shape[1] // 4
        key_s = projected[:, :tile] + block[:, latent_size:]
        key_l = projected[:, tile : 2 * tile]
        value_s = projected[:, 2 * tile : 3 * tile]
        value_l = projected[:, 3 * tile :]
        query_l = ql_ref[...]
        score_s = dot_t(qs_ref[...], key_s) * scale_s
        score_l = (dot_t(query_l[:, :tile], key_l) + dot_t(query_l[:, tile:], key_s)) * scale_l
        if first:
            row_pos = lax.broadcasted_iota(jnp.int32, (rows, rows), 0)
            key_pos = lax.broadcasted_iota(jnp.int32, (rows, rows), 1)
            allowed = key_pos <= row_pos
            score_s = jnp.where(allowed, score_s, masked_score)
            score_l = jnp.where(allowed, score_l, masked_score)
        for score, value, top, total, acc in (
            (score_s, value_s, max_s, sum_s, acc_s),
            (score_l, value_l, max_l, sum_l, acc_l),
        ):
            block_top = jnp.max(score, axis=1, keepdims=True)
            new_top = block_top if first else jnp.maximum(top[...], block_top)
            weights = jnp.exp(score - new_top)
            weight_sum = jnp.sum(weights, axis=1, keepdims=True)
            mixed = jnp.dot(
                weights.astype(jnp.bfloat16), value, preferred_element_type=jnp.float32
            )
            if first:
                total[...] = weight_sum
                acc[...] = mixed
            else:
                rescale = jnp.exp(top[...] - new_top)
                total[...] = total[...] * rescale + weight_sum
                acc[...] = acc[...] * rescale + mixed
            top[...] = new_top

    span(pack_ref[...], True)

    def pass_on(step, carry):
        @pl.when(step <= me_s)
        def _():
            source = me_s - step
            gather_copy(step, source, me_s).wait_recv()
            y_copy(step, source, me_t).start()
            c_copy(step, source, me_t).start()

        @pl.when((step >= 2) & (step <= me_s + 1))
        def _():
            before = step - 1
            source = me_s - before
            y_copy(before, source, y_t).wait_recv()
            d_copy(before, source, y_t).start()

        @pl.when(step >= 3)
        def _():
            before = step - 2
            source = me_s - before
            c_copy(before, source, core_t).wait_recv()
            d_copy(before, source, far_t).wait_recv()
            span(lat[source], False)

        return carry

    lax.fori_loop(1, me_s + 3, pass_on, 0)

    value_s = out_s_ref.shape[0]
    heads_s = (acc_s[:, :value_s] / sum_s[...]).astype(jnp.bfloat16)
    heads_l = (acc_l[...] / sum_l[...]).astype(jnp.bfloat16)
    part[...] = (
        jnp.dot(heads_s, out_s_ref[...], preferred_element_type=jnp.float32)
        + jnp.dot(heads_l, out_l_ref[...], preferred_element_type=jnp.float32)
    ).astype(jnp.bfloat16)

    def part_copy(number, target):
        return remote(
            part.at[rows_at(target, quarter), :],
            got.at[number],
            p_send.at[number],
            p_recv.at[number],
            me_s,
            target,
        )

    peers = (far_t, y_t, core_t)
    for number, peer in enumerate(peers):
        part_copy(number, peer).start()
    total = part[rows_at(me_t, quarter), :].astype(jnp.float32)
    for number, peer in reversed(tuple(enumerate(peers))):
        part_copy(number, peer).wait_recv()
        total = total + got[number].astype(jnp.float32)
    attention = total.astype(jnp.bfloat16).astype(jnp.float32)
    middle_ref[...] = (residual_ref[...].astype(jnp.float32) + attention).astype(jnp.bfloat16)

    for number, peer in enumerate(peers):
        part_copy(number, peer).wait_send()

    def drain_gather(step, carry):
        gather_copy(step, me_s, me_s + step).wait_send()
        return carry

    lax.fori_loop(1, n_sp - me_s, drain_gather, 0)

    def drain_shared(step, carry):
        source = me_s - step
        y_copy(step, source, me_t).wait_send()
        c_copy(step, source, me_t).wait_send()
        d_copy(step, source, y_t).wait_send()
        return carry

    lax.fori_loop(1, me_s + 1, drain_shared, 0)


def expert_kernel(
    n_sp,
    n_tp,
    capacity,
    middle_ref,
    gain_ref,
    routing_ref,
    route_weight_ref,
    gate_hbm,
    up_hbm,
    down_hbm,
    out_ref,
    gate_v,
    up_v,
    down_v,
    outgoing,
    recv,
    part,
    pair,
    y_out,
    y_in,
    back_out,
    back_in,
    w_sem,
    a_send,
    a_recv,
    y_send,
    y_recv,
    c_send,
    c_recv,
    d_send,
    d_recv,
    p_send,
    p_recv,
    z_send,
    z_recv,
    b_send,
    b_recv,
):
    me_s = lax.axis_index("sp")
    me_t = lax.axis_index("tp")
    core_t = me_t + 1 - 2 * (me_t % 2)
    y_t = (me_t + 2) % n_tp
    my_core = me_t % 2
    my_y = me_t // 2
    tok_count, width = middle_ref.shape
    slots = n_sp * capacity
    loads = (
        pltpu.make_async_copy(gate_hbm.at[0], gate_v, w_sem.at[0]),
        pltpu.make_async_copy(up_hbm.at[0], up_v, w_sem.at[1]),
        pltpu.make_async_copy(down_hbm.at[0], down_v, w_sem.at[2]),
    )
    for load in loads:
        load.start()

    normed = rms_scaled(middle_ref[...], gain_ref[...]).astype(jnp.bfloat16)
    routing = routing_ref[...]
    expert_ids = lax.broadcasted_iota(jnp.int32, (tok_count, slots), 1)
    named = [
        (routing[:, k : k + 1] == expert_ids).astype(jnp.float32) for k in range(TOPK)
    ]
    earlier = (
        lax.broadcasted_iota(jnp.int32, (tok_count, tok_count), 1)
        < lax.broadcasted_iota(jnp.int32, (tok_count, tok_count), 0)
    ).astype(jnp.bfloat16)
    ahead = jnp.dot(
        earlier, sum(named).astype(jnp.bfloat16), preferred_element_type=jnp.float32
    )
    picks = []
    for k in range(TOPK):
        slot = jnp.sum(named[k] * ahead, axis=1, keepdims=True).astype(jnp.int32)
        picks.append(
            (routing[:, k : k + 1] * capacity + slot == expert_ids).astype(jnp.float32)
        )
    send_table = jnp.transpose(sum(picks)).astype(jnp.bfloat16)
    outgoing[...] = jnp.dot(
        send_table, normed, preferred_element_type=jnp.float32
    ).astype(jnp.bfloat16)

    greet(n_sp, (core_t, y_t), me_s, me_t)

    def block(owner, source):
        return pl.ds(pl.multiple_of(owner * slots + source * capacity, capacity), capacity)

    def a_copy(step, source, target):
        return remote(
            outgoing.at[rows_at(target, capacity), :],
            recv.at[block(me_t, source), :],
            a_send.at[step],
            a_recv.at[step],
            target,
            me_t,
        )

    def shared(send, got, step, owner, target):
        where = recv.at[block(owner, (me_s + n_sp - step) % n_sp), :]
        return remote(where, where, send.at[step], got.at[step], me_s, target)

    for step in range(1, n_sp):
        a_copy(step, me_s, (me_s + step) % n_sp).start()
    recv[block(me_t, me_s), :] = outgoing[rows_at(me_s, capacity), :]
    for step in range(n_sp):
        if step:
            a_copy(step, (me_s + n_sp - step) % n_sp, me_s).wait_recv()
        shared(y_send, y_recv, step, me_t, y_t).start()
        shared(c_send, c_recv, step, me_t, core_t).start()
        if step:
            shared(y_send, y_recv, step - 1, y_t, y_t).wait_recv()
            shared(d_send, d_recv, step - 1, y_t, core_t).start()
    shared(y_send, y_recv, n_sp - 1, y_t, y_t).wait_recv()
    shared(d_send, d_recv, n_sp - 1, y_t, core_t).start()
    for load in loads:
        load.wait()

    half = 2 * slots

    def hidden_of(y_index):
        rows_in = recv[rows_at(y_index, half), :]
        gate_pre = jnp.dot(rows_in, gate_v[...], preferred_element_type=jnp.float32)
        up_pre = jnp.dot(rows_in, up_v[...], preferred_element_type=jnp.float32)
        return clamped(gate_pre, up_pre).astype(jnp.bfloat16)

    def down_of(y_index, hidden):
        part[rows_at(y_index, half), :] = jnp.dot(
            hidden, down_v[...], preferred_element_type=jnp.float32
        ).astype(jnp.bfloat16)

    def pair_copy(number, y_index, core_index):
        return remote(
            part.at[rows_at(2 * y_index + core_index, slots), :],
            pair.at[number],
            p_send.at[number],
            p_recv.at[number],
            me_s,
            core_t,
        )

    far_core = 1 - my_core
    far_y = 1 - my_y
    for step in range(n_sp):
        shared(d_send, d_recv, step, 2 * far_y + far_core, core_t).wait_recv()
    down_of(far_y, hidden_of(far_y))
    pair_copy(0, far_y, far_core).start()
    for step in range(n_sp):
        shared(c_send, c_recv, step, core_t, core_t).wait_recv()
    hidden = hidden_of(my_y)
    pair_copy(0, far_y, far_core).wait_recv()
    y_out[...] = (
        part[rows_at(y_t, slots), :].astype(jnp.float32) + pair[0].astype(jnp.float32)
    ).astype(jnp.bfloat16)

    def z_copy(step):
        where = rows_at((me_s + step) % n_sp, capacity)
        return remote(
            y_out.at[where, :], y_in.at[where, :], z_send.at[step], z_recv.at[step], me_s, y_t
        )

    order = tuple(range(1, n_sp)) + (0,)
    for step in order:
        z_copy(step).start()
    down_of(my_y, hidden)
    pair_copy(1, my_y, far_core).start()
    pair_copy(1, my_y, far_core).wait_recv()

    def back_copy(step, source, target):
        return remote(
            back_out.at[rows_at(target, capacity), :],
            back_in.at[rows_at(source, capacity), :],
            b_send.at[step],
            b_recv.at[step],
            target,
            me_t,
        )

    for step in order:
        target = (me_s + step) % n_sp
        z_copy(step).wait_recv()
        where = rows_at(target, capacity)
        summed = (
            part[block(me_t, target), :].astype(jnp.float32)
            + pair[1, where, :].astype(jnp.float32)
            + y_in[where, :].astype(jnp.float32)
        ).astype(jnp.bfloat16)
        if step:
            back_out[where, :] = summed
            back_copy(step, me_s, target).start()
        else:
            back_in[where, :] = summed
    for step in range(1, n_sp):
        back_copy(step, (me_s + n_sp - step) % n_sp, me_s).wait_recv()
    returned = back_in[...]
    mixed = middle_ref[...].astype(jnp.float32)
    route_weight = route_weight_ref[...]
    terms = [
        route_weight[:, k : k + 1]
        * jnp.dot(picks[k].astype(jnp.bfloat16), returned, preferred_element_type=jnp.float32)
        for k in range(TOPK)
    ]
    out_ref[...] = (mixed + sum(terms)).astype(jnp.bfloat16)

    for step in range(1, n_sp):
        a_copy(step, me_s, (me_s + step) % n_sp).wait_send()
        back_copy(step, me_s, (me_s + step) % n_sp).wait_send()
    for step in range(n_sp):
        shared(y_send, y_recv, step, me_t, y_t).wait_send()
        shared(c_send, c_recv, step, me_t, core_t).wait_send()
        shared(d_send, d_recv, step, y_t, core_t).wait_send()
        z_copy(step).wait_send()
    pair_copy(0, far_y, far_core).wait_send()
    pair_copy(1, my_y, far_core).wait_send()


def in_kernels(
    residual,
    query_small,
    query_large,
    latent,
    rotary_key,
    latent_gain,
    small_keys,
    small_values,
    large_keys,
    large_values,
    small_output,
    large_output,
    ffn_gain,
    gate_weights,
    up_weights,
    down_weights,
    routing,
    route_weight,
):
    n_sp, n_tp = lax.axis_size("sp"), lax.axis_size("tp")
    rows, latent_size = latent.shape
    tok_count, width = residual.shape
    hidden_units = gate_weights.shape[2]
    capacity = 2 * TOPK * tok_count // n_sp
    slots = n_sp * capacity
    half_rows = 2 * slots
    tile = NOPE_L
    first_pos = lax.axis_index("sp") * rows
    cos_vals, sin_vals = rope_tables(rows, first_pos)
    small_query = turn_queries(query_small, NOPE_S, cos_vals, sin_vals)[:, 0]
    large_query = turn_queries(query_large, NOPE_L, cos_vals, sin_vals)[:, 0]
    after = tile - NOPE_S - ROPE
    qs = jnp.pad(small_query, ((0, 0), (0, after)))
    ql = jnp.concatenate(
        [large_query[:, :NOPE_L], jnp.pad(large_query[:, NOPE_L:], ((0, 0), (NOPE_S, after)))],
        axis=1,
    )
    turned = rotate(rotary_key.astype(jnp.float32), cos_vals, sin_vals).astype(jnp.bfloat16)
    pack = jnp.concatenate(
        [
            rms_scaled(latent, latent_gain).astype(jnp.bfloat16),
            jnp.pad(turned, ((0, 0), (NOPE_S, after))),
        ],
        axis=1,
    )
    proj = jnp.concatenate(
        [
            jnp.pad(small_keys, ((0, 0), (0, tile - small_keys.shape[1]))),
            large_keys,
            jnp.pad(small_values, ((0, 0), (0, tile - small_values.shape[1]))),
            large_values,
        ],
        axis=1,
    )
    in_vmem = pl.BlockSpec(memory_space=pltpu.VMEM)
    in_hbm = pl.BlockSpec(memory_space=pltpu.HBM)
    dma = pltpu.SemaphoreType.DMA
    f32, bf16 = jnp.float32, jnp.bfloat16
    middle = pl.pallas_call(
        functools.partial(
            attention_kernel,
            n_sp,
            n_tp,
            (NOPE_S + ROPE) ** (-0.5),
            (NOPE_L + ROPE) ** (-0.5),
        ),
        name="attend",
        out_shape=jax.ShapeDtypeStruct(residual.shape, bf16),
        in_specs=[in_vmem] * 7,
        out_specs=in_vmem,
        scratch_shapes=[
            pltpu.VMEM((n_sp,) + pack.shape, bf16),
            pltpu.VMEM((rows, 1), f32),
            pltpu.VMEM((rows, 1), f32),
            pltpu.VMEM((rows, tile), f32),
            pltpu.VMEM((rows, 1), f32),
            pltpu.VMEM((rows, 1), f32),
            pltpu.VMEM((rows, tile), f32),
            pltpu.VMEM((rows, width), bf16),
            pltpu.VMEM((n_tp - 1, tok_count, width), bf16),
        ]
        + [dma((n_sp - 1,))] * 8
        + [dma((n_tp - 1,))] * 2,
        compiler_params=pltpu.CompilerParams(
            collective_id=0, has_side_effects=True, vmem_limit_bytes=24 * 2**20
        ),
    )(pack, qs, ql, proj, small_output, large_output, residual)
    return pl.pallas_call(
        functools.partial(expert_kernel, n_sp, n_tp, capacity),
        name="experts",
        out_shape=jax.ShapeDtypeStruct(residual.shape, bf16),
        in_specs=[in_vmem] * 4 + [in_hbm] * 3,
        out_specs=in_vmem,
        scratch_shapes=[
            pltpu.VMEM((width, hidden_units), bf16),
            pltpu.VMEM((width, hidden_units), bf16),
            pltpu.VMEM((hidden_units, width), bf16),
            pltpu.VMEM((slots, width), bf16),
            pltpu.VMEM((n_tp * slots, width), bf16),
            pltpu.VMEM((n_tp * slots, width), bf16),
            pltpu.VMEM((2, slots, width), bf16),
            pltpu.VMEM((slots, width), bf16),
            pltpu.VMEM((slots, width), bf16),
            pltpu.VMEM((slots, width), bf16),
            pltpu.VMEM((slots, width), bf16),
            dma((3,)),
        ]
        + [dma((n_sp,))] * 8
        + [dma((2,))] * 2
        + [dma((n_sp,))] * 4,
        compiler_params=pltpu.CompilerParams(
            collective_id=1, has_side_effects=True, vmem_limit_bytes=48 * 2**20
        ),
    )(
        middle,
        ffn_gain.reshape(1, width),
        routing,
        route_weight,
        gate_weights,
        up_weights,
        down_weights,
    )


def choose(*args):
    residual, latent, gate_weights = args[0], args[3], args[13]
    n_sp, n_tp = lax.axis_size("sp"), lax.axis_size("tp")
    tok_count = residual.shape[0]
    capacity = 2 * TOPK * tok_count // (n_sp * gate_weights.shape[0])
    fits = (
        n_tp == 4
        and gate_weights.shape[0] == 1
        and capacity > 0
        and capacity % 16 == 0
        and n_sp * capacity % 128 == 0
        and tok_count % 16 == 0
        and args[6].shape[1] == NOPE_S
        and args[8].shape[1] == NOPE_L
    )
    return in_kernels(*args) if fits else on_device(*args)


def solution(mesh):
    return jax.shard_map(
        choose,
        mesh=mesh,
        in_specs=(
            P(("sp", "tp"), None),
            P("sp", "tp"),
            P("sp", "tp"),
            P("sp", None),
            P("sp", None),
            P(),
            P(None, "tp"),
            P(None, "tp"),
            P(None, "tp"),
            P(None, "tp"),
            P("tp", None),
            P("tp", None),
            P(),
            P("sp", None, "tp"),
            P("sp", None, "tp"),
            P("sp", "tp", None),
            P(("sp", "tp"), None),
            P(("sp", "tp"), None),
        ),
        out_specs=P(("sp", "tp"), None),
        check_vma=False,
    )
```

```python
import functools

import jax
import jax.numpy as jnp
import numpy as np
from jax import lax
from jax.experimental import pallas as pl
from jax.experimental.pallas import tpu as pltpu
from jax.sharding import PartitionSpec as P

NOPE_S = 64
NOPE_L = 128
ROPE = 32
TOPK = 2


eps = 1e-06
clamp_limit = 7.0
glu_alpha = 1.702
rope_base = 10000.0
masked_score = -1e30


def rope_tables(row_count, first_pos):
    half_size = ROPE // 2
    frequencies = jnp.power(rope_base, -jnp.arange(half_size, dtype=jnp.float32) * (2.0 / ROPE))
    places = (first_pos + jnp.arange(row_count, dtype=jnp.int32)).astype(jnp.float32)
    angles = places[:, None] * frequencies[None, :]
    return (jnp.cos(angles), jnp.sin(angles))


def rotate(values_in, cos_vals, sin_vals):
    front_half, back_half = jnp.split(values_in, 2, axis=-1)
    return jnp.concatenate(
        [
            front_half * cos_vals - back_half * sin_vals,
            back_half * cos_vals + front_half * sin_vals,
        ],
        axis=-1,
    )


def rms_scaled(values_in, gain):
    widened = values_in.astype(jnp.float32)
    return widened * lax.rsqrt(jnp.mean(widened * widened, axis=-1, keepdims=True) + eps) * gain


def turn_queries(query, nope, cos_vals, sin_vals):
    width = nope + ROPE
    shaped = query.reshape(query.shape[0], query.shape[1] // width, width)
    turned = rotate(
        shaped[:, :, nope:].astype(jnp.float32), cos_vals[:, None, :], sin_vals[:, None, :]
    )
    return jnp.concatenate([shaped[:, :, :nope], turned.astype(jnp.bfloat16)], axis=2)


def clamped(gate_pre, up_pre):
    limited = jnp.minimum(gate_pre, clamp_limit)
    linear = jnp.clip(up_pre, -clamp_limit, clamp_limit)
    return limited * jax.nn.sigmoid(glu_alpha * limited) * (linear + 1.0)


def make_keys(latent_rows, raw_rotary, first_pos, latent_gain, projections):
    normed_latent = rms_scaled(latent_rows, latent_gain).astype(jnp.bfloat16)
    projected = tuple(
        (
            jnp.dot(normed_latent, weight, preferred_element_type=jnp.float32).astype(jnp.bfloat16)
            for weight in projections
        )
    )
    cos_vals, sin_vals = rope_tables(latent_rows.shape[0], first_pos)
    turned = rotate(raw_rotary.astype(jnp.float32), cos_vals, sin_vals).astype(jnp.bfloat16)
    return projected + (turned,)


def empty_state(query, values_in):
    head_count = query.shape[1]
    row_count = query.shape[0]
    value_size = values_in.shape[1] // head_count
    return (
        jnp.full((head_count, row_count), masked_score, jnp.float32),
        jnp.zeros((head_count, row_count), jnp.float32),
        jnp.zeros((row_count, head_count, value_size), jnp.float32),
    )


def update(state_now, query, keys_in, values_in, rotary, nope, allowed):
    running_max, weight_sum, weighted = state_now
    head_count = query.shape[1]
    span_rows = rotary.shape[0]
    key_heads = keys_in.reshape(span_rows, head_count, nope)
    value_heads = values_in.reshape(span_rows, head_count, -1)
    scores = jnp.einsum(
        "rhd,khd->hrk", query[:, :, :nope], key_heads, preferred_element_type=jnp.float32
    )
    scores = scores + jnp.einsum(
        "rhd,kd->hrk", query[:, :, nope:], rotary, preferred_element_type=jnp.float32
    )
    scores = jnp.where(allowed[None], scores * (nope + ROPE) ** (-0.5), masked_score)
    new_max = jnp.maximum(running_max, jnp.max(scores, axis=2))
    weights = jnp.where(allowed[None], jnp.exp(scores - new_max[:, :, None]), 0.0)
    rescale = jnp.exp(running_max - new_max)
    weight_sum = jnp.sum(weights, axis=2)
    weighted = weighted * rescale.T[:, :, None] + jnp.einsum(
        "hrk,khd->rhd",
        weights.astype(jnp.bfloat16),
        value_heads,
        preferred_element_type=jnp.float32,
    )
    return (new_max, weight_sum, weighted)


def finish(state_end, row_count):
    running_max, weight_sum, weighted = state_end
    return (weighted / weight_sum.T[:, :, None]).reshape(row_count, -1).astype(jnp.bfloat16)


def on_device(
    residual,
    query_small,
    query_large,
    latent,
    rotary_key,
    latent_gain,
    small_keys,
    small_values,
    large_keys,
    large_values,
    small_output,
    large_output,
    ffn_gain,
    gate_weights,
    up_weights,
    down_weights,
    routing,
    route_weight,
):
    row_count = latent.shape[0]
    first_pos = lax.axis_index("sp") * row_count
    cos_vals, sin_vals = rope_tables(row_count, first_pos)
    small_query = turn_queries(query_small, NOPE_S, cos_vals, sin_vals)
    large_query = turn_queries(query_large, NOPE_L, cos_vals, sin_vals)
    query_pos = first_pos + jnp.arange(row_count, dtype=jnp.int32)
    last_pos = first_pos + row_count - 1
    projections = (small_keys, small_values, large_keys, large_values)
    initial = (empty_state(small_query, small_values), empty_state(large_query, large_values))

    def from_latent(key_set, offset):
        return make_keys(key_set[0], key_set[1], offset, latent_gain, projections)

    key_set = (
        lax.all_gather(latent, "sp", axis=0, tiled=True),
        lax.all_gather(rotary_key, "sp", axis=0, tiled=True),
    )
    offset = jnp.int32(0)
    span_rows = key_set[0].shape[0]
    allowed = jnp.arange(span_rows, dtype=jnp.int32)[None, :] <= query_pos[:, None]

    def live(inner):
        ready = from_latent(key_set, offset)
        return (
            update(inner[0], small_query, ready[0], ready[1], ready[4], NOPE_S, allowed),
            update(inner[1], large_query, ready[2], ready[3], ready[4], NOPE_L, allowed),
        )

    def keep_state(inner):
        return inner

    state_end = lax.cond(offset <= last_pos, live, keep_state, initial)
    small_heads = finish(state_end[0], row_count)
    large_heads = finish(state_end[1], row_count)
    tok_count = row_count // lax.axis_size("tp")
    summed = lax.psum_scatter(
        (
            jnp.dot(small_heads, small_output, preferred_element_type=jnp.float32)
            + jnp.dot(large_heads, large_output, preferred_element_type=jnp.float32)
        ).astype(jnp.bfloat16),
        "tp",
        scatter_dimension=0,
        tiled=True,
    )
    attention = lax.optimization_barrier(summed).astype(jnp.float32)
    middle = lax.optimization_barrier(
        (residual.astype(jnp.float32) + attention).astype(jnp.bfloat16)
    )
    normed = rms_scaled(middle, ffn_gain).astype(jnp.bfloat16)
    local_experts = gate_weights.shape[0]
    expert_count = local_experts * lax.axis_size("sp")
    capacity = max(2, 2 * TOPK * tok_count // expert_count)
    assigned = routing.reshape(-1)
    onehot = (assigned[:, None] == jnp.arange(expert_count, dtype=jnp.int32)[None, :]).astype(
        jnp.int32
    )
    slot_index = jnp.sum((jnp.cumsum(onehot, axis=0) - onehot) * onehot, axis=1)
    places = assigned * capacity + slot_index
    pick_table = (
        places[:, None] == jnp.arange(expert_count * capacity, dtype=jnp.int32)[None, :]
    ).astype(jnp.bfloat16)
    send_table = jnp.sum(pick_table.reshape(tok_count, TOPK, -1), axis=1)
    outgoing = lax.dot_general(
        send_table, normed, (((0,), (0,)), ((), ())), preferred_element_type=jnp.float32
    )
    outgoing = outgoing.astype(jnp.bfloat16).reshape(expert_count, capacity, -1)
    shard_piece = lax.all_gather(
        lax.all_to_all(outgoing, "sp", split_axis=0, concat_axis=0, tiled=True),
        "tp",
        axis=0,
        tiled=True,
    )
    grouped = shard_piece.reshape(-1, local_experts, shard_piece.shape[1], shard_piece.shape[2])
    gate_pre = jnp.einsum(
        "secd,edf->secf", grouped, gate_weights, preferred_element_type=jnp.float32
    )
    up_pre = jnp.einsum("secd,edf->secf", grouped, up_weights, preferred_element_type=jnp.float32)
    hidden = clamped(gate_pre, up_pre).astype(jnp.bfloat16)
    result = jnp.einsum("secf,efd->secd", hidden, down_weights, preferred_element_type=jnp.float32)
    partials = result.reshape(shard_piece.shape[0], shard_piece.shape[1], -1)
    combined = lax.psum_scatter(
        partials.astype(jnp.bfloat16), "tp", scatter_dimension=0, tiled=True
    )
    returned = lax.all_to_all(combined, "sp", split_axis=0, concat_axis=0, tiled=True)
    picked = jnp.dot(
        pick_table,
        returned.reshape(expert_count * capacity, -1),
        preferred_element_type=jnp.float32,
    )
    mixed = jnp.sum(route_weight[:, :, None] * picked.reshape(tok_count, TOPK, -1), axis=1)
    return (middle.astype(jnp.float32) + mixed).astype(jnp.bfloat16)


MESH_ID = pl.DeviceIdType.MESH


def remote(src, dst, send_sem, recv_sem, sp, tp):
    return pltpu.make_async_remote_copy(
        src_ref=src,
        dst_ref=dst,
        send_sem=send_sem,
        recv_sem=recv_sem,
        device_id=(sp, tp),
        device_id_type=MESH_ID,
    )


def rows_at(index, count):
    return pl.ds(pl.multiple_of(index * count, count), count)


def greet(n_sp, tp_peers, me_s, me_t):
    barrier = pltpu.get_barrier_semaphore()
    for step in range(1, n_sp):
        pl.semaphore_signal(
            barrier, inc=1, device_id=((me_s + step) % n_sp, me_t), device_id_type=MESH_ID
        )
    for peer in tp_peers:
        pl.semaphore_signal(barrier, inc=1, device_id=(me_s, peer), device_id_type=MESH_ID)
    return lambda: pl.semaphore_wait(barrier, n_sp - 1 + len(tp_peers))


def dot_t(lhs, rhs):
    return lax.dot_general(
        lhs, rhs, (((1,), (1,)), ((), ())), preferred_element_type=jnp.float32
    )


def turned_rows(front, back, cos_vals, sin_vals):
    front, back = front.astype(jnp.float32), back.astype(jnp.float32)
    return jnp.concatenate(
        [front * cos_vals - back * sin_vals, back * cos_vals + front * sin_vals], axis=0
    )


def layer_kernel(
    n_sp,
    n_tp,
    capacity,
    latent_ref,
    rotary_ref,
    latent_gain_ref,
    cos_ref,
    sin_ref,
    qs_ref,
    ql_ref,
    keys_s_ref,
    values_s_ref,
    keys_l_ref,
    values_l_ref,
    out_s_ref,
    out_l_ref,
    residual_ref,
    gain_ref,
    routing_ref,
    route_weight_ref,
    gate_hbm,
    up_hbm,
    down_hbm,
    out_ref,
    pack_ref,
    lat,
    proj_ref,
    queries,
    scores,
    values,
    part_a,
    got,
    middle_ref,
    gate_v,
    up_v,
    down_v,
    outgoing,
    recv,
    part,
    pair,
    y_out,
    y_in,
    back_out,
    back_in,
    ga_send,
    ga_recv,
    gy_send,
    gy_recv,
    gc_send,
    gc_recv,
    gd_send,
    gd_recv,
    o_send,
    o_recv,
    w_sem,
    a_send,
    a_recv,
    y_send,
    y_recv,
    c_send,
    c_recv,
    d_send,
    d_recv,
    p_send,
    p_recv,
    z_send,
    z_recv,
    b_send,
    b_recv,
):
    me_s = lax.axis_index("sp")
    me_t = lax.axis_index("tp")
    core_t = me_t + 1 - 2 * (me_t % 2)
    y_t = (me_t + 2) % n_tp
    far_t = (core_t + 2) % n_tp
    rows, latent_size = latent_ref.shape
    tile = keys_l_ref.shape[1]
    quarter = rows // n_tp
    everyone = greet(n_sp, (core_t, y_t, far_t), me_s, me_t)
    loads = (
        pltpu.make_async_copy(gate_hbm.at[0], gate_v, w_sem.at[0]),
        pltpu.make_async_copy(up_hbm.at[0], up_v, w_sem.at[1]),
        pltpu.make_async_copy(down_hbm.at[0], down_v, w_sem.at[2]),
    )
    for load in loads:
        load.start()

    half_rope = ROPE // 2
    places = rows_at(me_s, rows)
    cos_vals, sin_vals = cos_ref[:, places], sin_ref[:, places]

    def rope_tile(ref, first):
        return turned_rows(
            ref[first : first + half_rope, :],
            ref[first + half_rope : first + ROPE, :],
            cos_vals,
            sin_vals,
        )

    def zero_rows(count, size):
        return jnp.zeros((count, size), jnp.float32)

    after = tile - NOPE_S - ROPE
    rotary_tile = jnp.concatenate(
        [zero_rows(NOPE_S, rows), rope_tile(rotary_ref, 0), zero_rows(after, rows)], axis=0
    )
    pack_ref[:, :latent_size] = rms_scaled(latent_ref[...], latent_gain_ref[...]).astype(
        jnp.bfloat16
    )
    pack_ref[:, latent_size:] = jnp.transpose(rotary_tile).astype(jnp.bfloat16)
    everyone()

    def gather_copy(step, source, target):
        return remote(
            pack_ref.at[rows_at(me_t, quarter), :],
            lat.at[source, rows_at(me_t, quarter), :],
            ga_send.at[step - 1],
            ga_recv.at[step - 1],
            target,
            me_t,
        )

    def share_copy(send, got_sem, step, source, owner, target):
        where = lat.at[source, rows_at(owner, quarter), :]
        return remote(where, where, send.at[step - 1], got_sem.at[step - 1], me_s, target)

    def y_copy(step, source, owner):
        return share_copy(gy_send, gy_recv, step, source, owner, y_t)

    def c_copy(step, source, owner):
        return share_copy(gc_send, gc_recv, step, source, owner, core_t)

    def d_copy(step, source, owner):
        return share_copy(gd_send, gd_recv, step, source, owner, core_t)

    def send_on(step, carry):
        gather_copy(step, me_s, me_s + step).start()
        return carry

    lax.fori_loop(1, n_sp - me_s, send_on, 0)

    query_s = jnp.concatenate(
        [
            qs_ref[:NOPE_S, :].astype(jnp.float32),
            rope_tile(qs_ref, NOPE_S),
            zero_rows(after, rows),
        ],
        axis=0,
    )
    query_l = jnp.concatenate(
        [zero_rows(NOPE_S, rows), rope_tile(ql_ref, NOPE_L), zero_rows(after, rows)], axis=0
    )
    queries[0] = jnp.transpose(query_s).astype(jnp.bfloat16)
    queries[1] = jnp.transpose(ql_ref[:NOPE_L, :].astype(jnp.float32)).astype(jnp.bfloat16)
    queries[2] = jnp.transpose(query_l).astype(jnp.bfloat16)
    for number, ref in ((0, keys_s_ref), (2, values_s_ref)):
        wide = jnp.concatenate(
            [ref[...].astype(jnp.float32), zero_rows(tile - ref.shape[0], latent_size)], axis=0
        )
        proj_ref[:, number * tile : (number + 1) * tile] = jnp.transpose(wide).astype(
            jnp.bfloat16
        )
    proj_ref[:, tile : 2 * tile] = keys_l_ref[...]
    proj_ref[:, 3 * tile :] = values_l_ref[...]
    scores[...] = jnp.full(scores.shape, masked_score, jnp.float32)
    values[...] = jnp.zeros(values.shape, jnp.bfloat16)
    scale_s = (NOPE_S + ROPE) ** (-0.5)
    scale_l = (NOPE_L + ROPE) ** (-0.5)

    def span(block_rows, source, first):
        projected = jnp.dot(
            block_rows[:, :latent_size], proj_ref[...], preferred_element_type=jnp.float32
        ).astype(jnp.bfloat16)
        key_s = projected[:, :tile] + block_rows[:, latent_size:]
        key_l = projected[:, tile : 2 * tile]
        where = rows_at(source, rows)
        values[where, :] = projected[:, 2 * tile :]
        score_s = dot_t(queries[0], key_s) * scale_s
        score_l = (dot_t(queries[1], key_l) + dot_t(queries[2], key_s)) * scale_l
        if first:
            row_pos = lax.broadcasted_iota(jnp.int32, (rows, rows), 0)
            key_pos = lax.broadcasted_iota(jnp.int32, (rows, rows), 1)
            allowed = key_pos <= row_pos
            score_s = jnp.where(allowed, score_s, masked_score)
            score_l = jnp.where(allowed, score_l, masked_score)
        scores[0, :, where] = score_s
        scores[1, :, where] = score_l

    span(pack_ref[...], me_s, True)

    def pass_on(step, carry):
        @pl.when(step <= me_s)
        def _():
            source = me_s - step
            gather_copy(step, source, me_s).wait_recv()
            y_copy(step, source, me_t).start()
            c_copy(step, source, me_t).start()

        @pl.when((step >= 2) & (step <= me_s + 1))
        def _():
            before = step - 1
            source = me_s - before
            y_copy(before, source, y_t).wait_recv()
            d_copy(before, source, y_t).start()

        @pl.when(step >= 3)
        def _():
            before = step - 2
            source = me_s - before
            c_copy(before, source, core_t).wait_recv()
            d_copy(before, source, far_t).wait_recv()
            span(lat[source], source, False)

        return carry

    lax.fori_loop(1, me_s + 3, pass_on, 0)

    def mixed_head(number):
        score = scores[number]
        top = jnp.max(score, axis=1, keepdims=True)
        weights = jnp.exp(score - top)
        total = jnp.sum(weights, axis=1, keepdims=True)
        summed = jnp.dot(
            weights.astype(jnp.bfloat16),
            values[:, number * tile : (number + 1) * tile],
            preferred_element_type=jnp.float32,
        )
        return (summed / total).astype(jnp.bfloat16)

    heads_s = mixed_head(0)[:, : out_s_ref.shape[0]]
    heads_l = mixed_head(1)
    part_a[...] = (
        jnp.dot(heads_s, out_s_ref[...], preferred_element_type=jnp.float32)
        + jnp.dot(heads_l, out_l_ref[...], preferred_element_type=jnp.float32)
    ).astype(jnp.bfloat16)

    def part_copy(number, target):
        return remote(
            part_a.at[rows_at(target, quarter), :],
            got.at[number],
            o_send.at[number],
            o_recv.at[number],
            me_s,
            target,
        )

    peers = (far_t, y_t, core_t)
    for number, peer in enumerate(peers):
        part_copy(number, peer).start()
    total = part_a[rows_at(me_t, quarter), :].astype(jnp.float32)
    for number, peer in reversed(tuple(enumerate(peers))):
        part_copy(number, peer).wait_recv()
        total = total + got[number].astype(jnp.float32)
    attention = total.astype(jnp.bfloat16).astype(jnp.float32)
    middle_ref[...] = (residual_ref[...].astype(jnp.float32) + attention).astype(jnp.bfloat16)

    my_core = me_t % 2
    my_y = me_t // 2
    tok_count, width = middle_ref.shape
    slots = n_sp * capacity
    normed = rms_scaled(middle_ref[...], gain_ref[...]).astype(jnp.bfloat16)
    routing = routing_ref[...]
    expert_ids = lax.broadcasted_iota(jnp.int32, (slots, tok_count), 0)
    named = [(routing[k : k + 1, :] == expert_ids).astype(jnp.float32) for k in range(TOPK)]
    earlier = (
        lax.broadcasted_iota(jnp.int32, (tok_count, tok_count), 0)
        < lax.broadcasted_iota(jnp.int32, (tok_count, tok_count), 1)
    ).astype(jnp.bfloat16)
    ahead = jnp.dot(
        sum(named).astype(jnp.bfloat16), earlier, preferred_element_type=jnp.float32
    )
    picks = []
    for k in range(TOPK):
        slot = jnp.sum(named[k] * ahead, axis=0, keepdims=True).astype(jnp.int32)
        picks.append(
            (routing[k : k + 1, :] * capacity + slot == expert_ids).astype(jnp.float32)
        )
    send_table = sum(picks).astype(jnp.bfloat16)
    outgoing[...] = jnp.dot(
        send_table, normed, preferred_element_type=jnp.float32
    ).astype(jnp.bfloat16)

    def block(owner, source):
        return pl.ds(pl.multiple_of(owner * slots + source * capacity, capacity), capacity)

    def a_copy(step, source, target):
        return remote(
            outgoing.at[rows_at(target, capacity), :],
            recv.at[block(me_t, source), :],
            a_send.at[step],
            a_recv.at[step],
            target,
            me_t,
        )

    def shared(send, got, step, owner, target):
        where = recv.at[block(owner, (me_s + n_sp - step) % n_sp), :]
        return remote(where, where, send.at[step], got.at[step], me_s, target)

    for step in range(1, n_sp):
        a_copy(step, me_s, (me_s + step) % n_sp).start()
    recv[block(me_t, me_s), :] = outgoing[rows_at(me_s, capacity), :]
    for step in range(n_sp):
        if step:
            a_copy(step, (me_s + n_sp - step) % n_sp, me_s).wait_recv()
        shared(y_send, y_recv, step, me_t, y_t).start()
        shared(c_send, c_recv, step, me_t, core_t).start()
        if step:
            shared(y_send, y_recv, step - 1, y_t, y_t).wait_recv()
            shared(d_send, d_recv, step - 1, y_t, core_t).start()
    shared(y_send, y_recv, n_sp - 1, y_t, y_t).wait_recv()
    shared(d_send, d_recv, n_sp - 1, y_t, core_t).start()
    for load in loads:
        load.wait()

    half = 2 * slots

    def hidden_of(y_index):
        rows_in = recv[rows_at(y_index, half), :]
        gate_pre = jnp.dot(rows_in, gate_v[...], preferred_element_type=jnp.float32)
        up_pre = jnp.dot(rows_in, up_v[...], preferred_element_type=jnp.float32)
        return clamped(gate_pre, up_pre).astype(jnp.bfloat16)

    def down_of(y_index, hidden):
        part[rows_at(y_index, half), :] = jnp.dot(
            hidden, down_v[...], preferred_element_type=jnp.float32
        ).astype(jnp.bfloat16)

    def pair_copy(number, y_index, core_index):
        return remote(
            part.at[rows_at(2 * y_index + core_index, slots), :],
            pair.at[number],
            p_send.at[number],
            p_recv.at[number],
            me_s,
            core_t,
        )

    far_core = 1 - my_core
    far_y = 1 - my_y
    for step in range(n_sp):
        shared(d_send, d_recv, step, 2 * far_y + far_core, core_t).wait_recv()
    down_of(far_y, hidden_of(far_y))
    pair_copy(0, far_y, far_core).start()
    for step in range(n_sp):
        shared(c_send, c_recv, step, core_t, core_t).wait_recv()
    hidden = hidden_of(my_y)
    pair_copy(0, far_y, far_core).wait_recv()
    y_out[...] = (
        part[rows_at(y_t, slots), :].astype(jnp.float32) + pair[0].astype(jnp.float32)
    ).astype(jnp.bfloat16)

    def z_copy(step):
        where = rows_at((me_s + step) % n_sp, capacity)
        return remote(
            y_out.at[where, :], y_in.at[where, :], z_send.at[step], z_recv.at[step], me_s, y_t
        )

    order = tuple(range(1, n_sp)) + (0,)
    for step in order:
        z_copy(step).start()
    down_of(my_y, hidden)
    pair_copy(1, my_y, far_core).start()
    pair_copy(1, my_y, far_core).wait_recv()

    def back_copy(step, source, target):
        return remote(
            back_out.at[rows_at(target, capacity), :],
            back_in.at[rows_at(source, capacity), :],
            b_send.at[step],
            b_recv.at[step],
            target,
            me_t,
        )

    for step in order:
        target = (me_s + step) % n_sp
        z_copy(step).wait_recv()
        where = rows_at(target, capacity)
        summed = (
            part[block(me_t, target), :].astype(jnp.float32)
            + pair[1, where, :].astype(jnp.float32)
            + y_in[where, :].astype(jnp.float32)
        ).astype(jnp.bfloat16)
        if step:
            back_out[where, :] = summed
            back_copy(step, me_s, target).start()
        else:
            back_in[where, :] = summed
    for step in range(1, n_sp):
        back_copy(step, (me_s + n_sp - step) % n_sp, me_s).wait_recv()
    returned = back_in[...]
    mixed = middle_ref[...].astype(jnp.float32)
    route_weight = route_weight_ref[...]
    terms = []
    for k in range(TOPK):
        weighted = jnp.transpose(picks[k] * route_weight[k : k + 1, :])
        terms.append(
            jnp.sum(weighted, axis=1, keepdims=True)
            * jnp.dot(
                jnp.transpose(picks[k]).astype(jnp.bfloat16),
                returned,
                preferred_element_type=jnp.float32,
            )
        )
    out_ref[...] = (mixed + sum(terms)).astype(jnp.bfloat16)

    for step in range(1, n_sp):
        a_copy(step, me_s, (me_s + step) % n_sp).wait_send()
        back_copy(step, me_s, (me_s + step) % n_sp).wait_send()
    for step in range(n_sp):
        shared(y_send, y_recv, step, me_t, y_t).wait_send()
        shared(c_send, c_recv, step, me_t, core_t).wait_send()
        shared(d_send, d_recv, step, y_t, core_t).wait_send()
        z_copy(step).wait_send()
    pair_copy(0, far_y, far_core).wait_send()
    pair_copy(1, my_y, far_core).wait_send()

    for number, peer in enumerate(peers):
        part_copy(number, peer).wait_send()

    def drain_gather(step, carry):
        gather_copy(step, me_s, me_s + step).wait_send()
        return carry

    lax.fori_loop(1, n_sp - me_s, drain_gather, 0)

    def drain_shared(step, carry):
        source = me_s - step
        y_copy(step, source, me_t).wait_send()
        c_copy(step, source, me_t).wait_send()
        d_copy(step, source, y_t).wait_send()
        return carry

    lax.fori_loop(1, me_s + 1, drain_shared, 0)


def in_kernels(
    residual,
    query_small,
    query_large,
    latent,
    rotary_key,
    latent_gain,
    small_keys,
    small_values,
    large_keys,
    large_values,
    small_output,
    large_output,
    ffn_gain,
    gate_weights,
    up_weights,
    down_weights,
    routing,
    route_weight,
):
    n_sp, n_tp = lax.axis_size("sp"), lax.axis_size("tp")
    rows, latent_size = latent.shape
    tok_count, width = residual.shape
    hidden_units = gate_weights.shape[2]
    capacity = 2 * TOPK * tok_count // n_sp
    slots = n_sp * capacity
    tile = NOPE_L
    frequencies = np.float32(rope_base) ** (
        -np.arange(ROPE // 2, dtype=np.float32) * np.float32(2.0 / ROPE)
    )
    places = np.arange(n_sp * rows, dtype=np.float32)
    angles = (frequencies[:, None] * places[None, :]).astype(np.float32)
    cos_table = jnp.asarray(np.cos(angles), jnp.float32)
    sin_table = jnp.asarray(np.sin(angles), jnp.float32)
    in_vmem = pl.BlockSpec(memory_space=pltpu.VMEM)
    in_hbm = pl.BlockSpec(memory_space=pltpu.HBM)
    dma = pltpu.SemaphoreType.DMA
    f32, bf16 = jnp.float32, jnp.bfloat16
    return pl.pallas_call(
        functools.partial(layer_kernel, n_sp, n_tp, capacity),
        name="layer",
        out_shape=jax.ShapeDtypeStruct(residual.shape, bf16),
        in_specs=[in_vmem] * 17 + [in_hbm] * 3,
        out_specs=in_vmem,
        scratch_shapes=[
            pltpu.VMEM((rows, latent_size + tile), bf16),
            pltpu.VMEM((n_sp, rows, latent_size + tile), bf16),
            pltpu.VMEM((latent_size, 4 * tile), bf16),
            pltpu.VMEM((3, rows, tile), bf16),
            pltpu.VMEM((2, rows, n_sp * rows), f32),
            pltpu.VMEM((n_sp * rows, 2 * tile), bf16),
            pltpu.VMEM((rows, width), bf16),
            pltpu.VMEM((n_tp - 1, tok_count, width), bf16),
            pltpu.VMEM((tok_count, width), bf16),
            pltpu.VMEM((width, hidden_units), bf16),
            pltpu.VMEM((width, hidden_units), bf16),
            pltpu.VMEM((hidden_units, width), bf16),
            pltpu.VMEM((slots, width), bf16),
            pltpu.VMEM((n_tp * slots, width), bf16),
            pltpu.VMEM((n_tp * slots, width), bf16),
            pltpu.VMEM((2, slots, width), bf16),
            pltpu.VMEM((slots, width), bf16),
            pltpu.VMEM((slots, width), bf16),
            pltpu.VMEM((slots, width), bf16),
            pltpu.VMEM((slots, width), bf16),
        ]
        + [dma((n_sp - 1,))] * 8
        + [dma((n_tp - 1,))] * 2
        + [dma((3,))]
        + [dma((n_sp,))] * 8
        + [dma((2,))] * 2
        + [dma((n_sp,))] * 4,
        compiler_params=pltpu.CompilerParams(
            collective_id=0, has_side_effects=True, vmem_limit_bytes=60 * 2**20
        ),
    )(
        latent,
        rotary_key.T,
        latent_gain.reshape(1, latent_size),
        cos_table,
        sin_table,
        query_small.T,
        query_large.T,
        small_keys.T,
        small_values.T,
        large_keys,
        large_values,
        small_output,
        large_output,
        residual,
        ffn_gain.reshape(1, width),
        routing.T,
        route_weight.T,
        gate_weights,
        up_weights,
        down_weights,
    )


def choose(*args):
    residual, latent, gate_weights = args[0], args[3], args[13]
    n_sp, n_tp = lax.axis_size("sp"), lax.axis_size("tp")
    tok_count = residual.shape[0]
    capacity = 2 * TOPK * tok_count // (n_sp * gate_weights.shape[0])
    fits = (
        n_tp == 4
        and gate_weights.shape[0] == 1
        and capacity > 0
        and capacity % 16 == 0
        and n_sp * capacity % 128 == 0
        and tok_count % 16 == 0
        and latent.shape[0] % 128 == 0
        and args[6].shape[1] == NOPE_S
        and args[8].shape[1] == NOPE_L
    )
    return in_kernels(*args) if fits else on_device(*args)


def solution(mesh):
    return jax.shard_map(
        choose,
        mesh=mesh,
        in_specs=(
            P(("sp", "tp"), None),
            P("sp", "tp"),
            P("sp", "tp"),
            P("sp", None),
            P("sp", None),
            P(),
            P(None, "tp"),
            P(None, "tp"),
            P(None, "tp"),
            P(None, "tp"),
            P("tp", None),
            P("tp", None),
            P(),
            P("sp", None, "tp"),
            P("sp", None, "tp"),
            P("sp", "tp", None),
            P(("sp", "tp"), None),
            P(("sp", "tp"), None),
        ),
        out_specs=P(("sp", "tp"), None),
        check_vma=False,
    )
```
